32 devices in a mesh: sp: 4 (over z), tp: 8 (over y, x, core).
Axes of the slice: x: 2, y: 2, z: 4, core: 2. Of those that a mesh axis runs over, the one named last changes fastest.
Arguments:
- latent: bfloat16 [3072, 4096], P('sp', 'tp'), may hold values from -600 to 600
- context: bfloat16 [512, 4096], P('sp', 'tp'), may hold values from -600 to 600
- cond: float32 [4096], P('sp'), may hold values from -6 to 6
- ctx_cond: float32 [4096], P('sp'), may hold values from -6 to 6
- w_shift: bfloat16 [4096, 4096], P('sp', 'tp'), may hold values from -0.09375 to 0.09375
- w_scale: bfloat16 [4096, 4096], P('sp', 'tp'), may hold values from -0.09375 to 0.09375
- w_gate: bfloat16 [4096, 4096], P('sp', 'tp'), may hold values from -0.1875 to 0.1875
- norm_gain: float32 [4096], P('tp'), may hold values from 0.1 to 1.9
- w_query: bfloat16 [2048, 4096], P('tp'), may hold values from -0.09375 to 0.09375
- w_key: bfloat16 [2048, 4096], P('tp'), may hold values from -0.09375 to 0.09375
- w_value: bfloat16 [4096, 4096], P('tp'), may hold values from -0.09375 to 0.09375
- w_decay_fwd: bfloat16 [2048, 4096], P('tp'), may hold values from -0.09375 to 0.09375
- w_decay_bwd: bfloat16 [2048, 4096], P('tp'), may hold values from -0.09375 to 0.09375
- forgetting_shift_vector: float32 [2048], P('tp')
- decay_log: float32 [3072, 64], P('sp', 'tp'), may hold values from -3 to 0
- head_gain: float32 [4096], P('tp'), may hold values from 0.1 to 1.9
- w_out: bfloat16 [4096, 4096], P('tp'), may hold values from -0.09375 to 0.09375
Outputs:
- update: bfloat16 [3072, 4096], P('sp', 'tp')
The draws below stay inside these ranges and needn't reach their ends.
All inputs are finite; a program needn't handle non-finite values.
Results may differ from the reference program's by a relative error of at most 0.012.
The reference program's roundings to bfloat16 on the way (of `heads_out`) count: a program that leaves them out, or rounds other values in their place, can miss the bound.
Values may be sent and summed in bfloat16 or wider, within the bound.
A program may use at most 128 MiB of HBM per device.

```python
import math
import jax
import jax.numpy as jnp
from jax import lax

WIDTH = 4096
HEADS = 64
ADDRESS_WIDTH = 32
VALUE_DIM = 64
BLOCK = 64
TOK_SP = 768
CTX = 512
SEQ = 3072
N_TP = 8


def activation_rows(key, count):
    pieces = jax.random.split(key, 3)
    channel = jnp.arange(WIDTH) // (WIDTH // N_TP)
    rising = channel.astype(jnp.float32) / max(N_TP - 1, 1)
    row_scale = jnp.exp(jax.random.uniform(pieces[0], (count, 1), jnp.float32, 0.0, math.log(10.0)))
    col_jitter = jnp.exp(jax.random.uniform(pieces[1], (1, WIDTH), jnp.float32, -0.35, 0.35))
    base = jnp.clip(jax.random.normal(pieces[2], (count, WIDTH), jnp.float32), -4.0, 4.0)
    col_rise = 3.0 ** rising
    return (base * row_scale * col_jitter * col_rise[None, :]).astype(jnp.bfloat16)


def draw_latent(key, part):
    return activation_rows(jax.random.fold_in(key, 11), SEQ)


def draw_context(key, part):
    return activation_rows(jax.random.fold_in(key, 12), CTX)


def draw_forgetting_shift_vector(key, part):
    pieces = jax.random.split(jax.random.fold_in(key, 13), 4)
    share = 0.5
    slow = jax.random.uniform(pieces[0], (HEADS, 1), jnp.float32) < share
    slow_level = math.log((CTX + SEQ) / 16.0) + jax.random.uniform(pieces[1], (HEADS, 1), jnp.float32, 0.5, 1.5)
    fast_level = jax.random.uniform(pieces[2], (HEADS, 1), jnp.float32, 0.3, 1.5)
    jitter = jax.random.uniform(pieces[3], (HEADS, ADDRESS_WIDTH), jnp.float32, -0.3, 0.3)
    return (jnp.where(slow, slow_level, fast_level) + jitter).reshape(HEADS * ADDRESS_WIDTH)


def draw_decay_log(key, part):
    pieces = jax.random.split(jax.random.fold_in(key, 14), 3)
    segments = SEQ // TOK_SP
    rates = jnp.exp(jax.random.uniform(pieces[0], (segments, 1, HEADS), jnp.float32, math.log(0.1), math.log(0.5))) / (CTX + SEQ)
    equilibrium_memory_matrix = jnp.broadcast_to(rates, (segments, TOK_SP, HEADS)).reshape(SEQ, HEADS)
    places = jax.random.randint(pieces[1], (3,), 0, SEQ)
    nesting_tiers = jnp.log(jax.random.uniform(pieces[2], (3,), jnp.float32, 0.5, 0.8))
    agreement_tally = (jnp.arange(SEQ)[:, None] == places[None, :]).astype(jnp.float32)
    cluster_partition = jnp.dot(agreement_tally, nesting_tiers)[:, None]
    return cluster_partition - equilibrium_memory_matrix


def shard_levels(rng, shape, shards, low, top_value):
    def one(axis_at, blocks):
        steps = jax.random.uniform(jax.random.fold_in(jax.random.fold_in(rng, 6), axis_at), (blocks,), jnp.float32, low / len(shards), top_value / len(shards))
        return jnp.repeat(jnp.exp(steps), shape[axis_at] // blocks).reshape((-1,) + (1,) * (len(shape) - axis_at - 1))

    gain = one(*shards[0])
    for cut in shards[1:]:
        gain = gain * one(*cut)
    return gain


def scatter_about(key, extent, width, limit, cuts=(), dtype=jnp.bfloat16):
    entries = width * jax.random.normal(key, extent, jnp.float32)
    if cuts:
        entries = entries * shard_levels(key, extent, cuts, -0.22, 0.18)
    return jnp.clip(entries, -limit, limit).astype(dtype)


def setup_inputs(seed: int = 0) -> dict:
    seeds = jax.random.split(jax.random.key(seed), 18)
    return {
        "latent": draw_latent(jax.random.fold_in(seeds[17], 71), 0),
        "context": draw_context(jax.random.fold_in(seeds[17], 71), 0),
        "cond": scatter_about(seeds[2], (WIDTH,), 1.0, 6.0, ((0, 4),), jnp.float32),
        "ctx_cond": scatter_about(seeds[3], (WIDTH,), 1.0, 6.0, ((0, 4),), jnp.float32),
        "w_shift": scatter_about(seeds[4], (WIDTH, WIDTH), WIDTH ** -0.5, 0.09375, ((0, 4), (1, 8))),
        "w_scale": scatter_about(seeds[5], (WIDTH, WIDTH), WIDTH ** -0.5, 0.09375, ((0, 4), (1, 8))),
        "w_gate": scatter_about(seeds[6], (WIDTH, WIDTH), (WIDTH // 4) ** -0.5, 0.1875, ((0, 4), (1, 8))),
        "norm_gain": jnp.clip(1.0 + 0.18 * jax.random.normal(seeds[7], (WIDTH,), jnp.float32), 0.1, 1.9),
        "w_query": scatter_about(seeds[8], (HEADS * ADDRESS_WIDTH, WIDTH), WIDTH ** -0.5, 0.09375, ((0, 8),)),
        "w_key": scatter_about(seeds[9], (HEADS * ADDRESS_WIDTH, WIDTH), WIDTH ** -0.5, 0.09375, ((0, 8),)),
        "w_value": scatter_about(seeds[10], (HEADS * VALUE_DIM, WIDTH), WIDTH ** -0.5, 0.09375, ((0, 8),)),
        "w_decay_fwd": scatter_about(seeds[11], (HEADS * ADDRESS_WIDTH, WIDTH), WIDTH ** -0.5, 0.09375, ((0, 8),)),
        "w_decay_bwd": scatter_about(seeds[12], (HEADS * ADDRESS_WIDTH, WIDTH), WIDTH ** -0.5, 0.09375, ((0, 8),)),
        "forgetting_shift_vector": draw_forgetting_shift_vector(jax.random.fold_in(seeds[17], 71), 0),
        "decay_log": draw_decay_log(jax.random.fold_in(seeds[17], 71), 0),
        "head_gain": jnp.clip(1.0 + 0.18 * jax.random.normal(seeds[15], (HEADS * VALUE_DIM,), jnp.float32), 0.1, 1.9),
        "w_out": scatter_about(seeds[16], (WIDTH, HEADS * VALUE_DIM), (HEADS * VALUE_DIM) ** -0.5, 0.09375, ((0, 8),)),
    }


epsilon = 1e-06
smoothing_scale_factor = 16.0
highest_precision = lax.Precision.HIGHEST

def rounded(matrix):
    return lax.optimization_barrier(matrix.astype(jnp.bfloat16)).astype(jnp.float32)

def contract(left, right):
    return lax.dot_general(left, right, (((1,), (1,)), ((), ())), preferred_element_type=jnp.float32)

def divide_among_attention_units(matrix, head_width):
    return jnp.transpose(matrix.reshape(matrix.shape[0], -1, head_width), (1, 0, 2))

def blockwise(query_rows, key_rows, value_rows, log_decay, initial_state):
    head_count, length, key_width = query_rows.shape
    block_count = length // BLOCK

    def to_blocks(tensor):
        return jnp.moveaxis(tensor.reshape(head_count, block_count, BLOCK, tensor.shape[-1]), 1, 0)
    lower_mask = jnp.tril(jnp.ones((BLOCK, BLOCK), jnp.float32))

    def advance(current_state, inputs):
        query_block, key_block_rows, value_block_rows, decay_block = inputs
        cumulative_logs = jnp.cumsum(decay_block, axis=1)
        block_finish = cumulative_logs[:, -1:, :]
        decayed_query_rows = query_block * jnp.exp(cumulative_logs)
        scores = jnp.einsum('hck,hsk->hcs', decayed_query_rows, key_block_rows * jnp.exp(-cumulative_logs), precision=highest_precision) * lower_mask
        output_rows = jnp.einsum('hcs,hsv->hcv', scores, value_block_rows, precision=highest_precision)
        output_rows = output_rows + jnp.einsum('sei,siw->sew', decayed_query_rows, current_state, precision=highest_precision)
        current_state = jnp.exp(block_finish[:, 0, :])[:, :, None] * current_state + jnp.einsum('zoa,zol->zal', key_block_rows * jnp.exp(block_finish - cumulative_logs), value_block_rows, precision=highest_precision)
        return (current_state, output_rows)
    final_state, outputs = lax.scan(advance, initial_state, (to_blocks(query_rows), to_blocks(key_rows), to_blocks(value_rows), to_blocks(log_decay)))
    return (jnp.moveaxis(outputs, 0, 1).reshape(head_count, length, -1), final_state)

def project(rows, norm_gain, shift, scale, weights):
    wide = rows.astype(jnp.float32)
    inverse = lax.rsqrt(lax.optimization_barrier(jnp.sum(wide * wide, axis=1, keepdims=True)) / WIDTH + epsilon)
    scaled = (wide * (norm_gain * (1.0 + scale))[None, :]).astype(jnp.bfloat16)
    shift_row = shift.astype(jnp.bfloat16)[None, :]
    return [inverse * contract(scaled, weight) + contract(shift_row, weight) for weight in weights]

def reference(latent, context, cond, ctx_cond, w_shift, w_scale, w_gate, norm_gain, w_query, w_key, w_value, w_decay_fwd, w_decay_bwd, forgetting_shift_vector, decay_log, head_gain, w_out):
    act_lat = jax.nn.silu(cond).astype(jnp.bfloat16)[None, :]
    act_ctx = jax.nn.silu(ctx_cond).astype(jnp.bfloat16)[None, :]
    shift_lat = jnp.dot(act_lat, w_shift, preferred_element_type=jnp.float32)[0]
    scale_lat = jnp.dot(act_lat, w_scale, preferred_element_type=jnp.float32)[0]
    gate_lat = jnp.dot(act_lat, w_gate, preferred_element_type=jnp.float32)[0]
    shift_ctx = jnp.dot(act_ctx, w_shift, preferred_element_type=jnp.float32)[0]
    scale_ctx = jnp.dot(act_ctx, w_scale, preferred_element_type=jnp.float32)[0]
    pre_query, pre_key, pre_value, onward_leading_sums, reverse_leading_sums = project(latent, norm_gain, shift_lat, scale_lat, (w_query, w_key, w_value, w_decay_fwd, w_decay_bwd))
    cpre_key, cpre_value, conditioning_onward_leading, conditioning_reverse_leading = project(context, norm_gain, shift_ctx, scale_ctx, (w_key, w_value, w_decay_fwd, w_decay_bwd))
    query_rows = divide_among_attention_units(rounded(pre_query), ADDRESS_WIDTH) * ADDRESS_WIDTH ** (-0.5)
    key_lat = divide_among_attention_units(rounded(pre_key), ADDRESS_WIDTH)
    value_lat = divide_among_attention_units(rounded(pre_value), VALUE_DIM)
    context_key_rows = divide_among_attention_units(rounded(cpre_key), ADDRESS_WIDTH)
    context_value_rows = divide_among_attention_units(rounded(cpre_value), VALUE_DIM)
    summand_list = jnp.transpose(decay_log)[:, :, None]
    onward_logarithms = divide_among_attention_units(jax.nn.log_sigmoid(onward_leading_sums + forgetting_shift_vector[None, :]) / smoothing_scale_factor, ADDRESS_WIDTH) + summand_list
    reverse_logarithms = divide_among_attention_units(jax.nn.log_sigmoid(reverse_leading_sums + forgetting_shift_vector[None, :]) / smoothing_scale_factor, ADDRESS_WIDTH) + summand_list
    conditioning_onward_logarithms = divide_among_attention_units(jax.nn.log_sigmoid(conditioning_onward_leading + forgetting_shift_vector[None, :]) / smoothing_scale_factor, ADDRESS_WIDTH)
    conditioning_reverse_logarithms = divide_among_attention_units(jax.nn.log_sigmoid(conditioning_reverse_leading + forgetting_shift_vector[None, :]) / smoothing_scale_factor, ADDRESS_WIDTH)
    cumulative_forward = jnp.cumsum(conditioning_onward_logarithms, axis=1)
    context_forward = jnp.einsum('xcq,xcs->xqs', context_key_rows * jnp.exp(cumulative_forward[:, -1:, :] - cumulative_forward), context_value_rows, precision=highest_precision)
    cumulative_backward = jnp.cumsum(conditioning_reverse_logarithms, axis=1)
    context_backward = jnp.einsum('xcq,xcs->xqs', context_key_rows * jnp.exp(cumulative_backward - conditioning_reverse_logarithms), context_value_rows, precision=highest_precision)
    fwd_out, unused_fwd = blockwise(query_rows, key_lat, value_lat, onward_logarithms, context_forward)
    bwd_flip, unused_bwd = blockwise(jnp.flip(query_rows, 1), jnp.flip(key_lat, 1), jnp.flip(value_lat, 1), jnp.flip(reverse_logarithms, 1), context_backward)
    mixed = fwd_out + jnp.flip(bwd_flip, 1)
    normed = mixed * lax.rsqrt(lax.optimization_barrier(jnp.mean(mixed * mixed, axis=2, keepdims=True)) + epsilon)
    normed = normed * head_gain.reshape(HEADS, 1, VALUE_DIM)
    heads_out = jnp.transpose(normed, (1, 0, 2)).reshape(SEQ, HEADS * VALUE_DIM).astype(jnp.bfloat16)
    projected = contract(heads_out, w_out)
    return (gate_lat[None, :] * projected).astype(jnp.bfloat16)
```

```python
import functools

import jax
import jax.numpy as jnp
from jax import lax
from jax.experimental import pallas as pl
from jax.experimental.pallas import tpu as pltpu
from jax.sharding import PartitionSpec as P

ADDRESS_WIDTH = 32
VALUE_DIM = 64
GROUP = 4
GK = GROUP * ADDRESS_WIDTH
GV = GROUP * VALUE_DIM
PAD = 16
LOG_ROWS = 8

epsilon = 1e-06
smoothing = 16.0
exact = lax.Precision.HIGHEST
F32 = jnp.float32
BF16 = jnp.bfloat16


def block_of(length):
    block = 128
    while length % block:
        block //= 2
    return block


def contract(left, right):
    return lax.dot_general(left, right, (((1,), (1,)), ((), ())), preferred_element_type=F32)


def outer(left, right):
    return lax.dot_general(left, right, (((0,), (0,)), ((), ())), preferred_element_type=F32)


def iota(shape, axis):
    return lax.broadcasted_iota(jnp.int32, shape, axis)


def diagonal_mask():
    return iota((GV, GK), 0) // VALUE_DIM == iota((GV, GK), 1) // ADDRESS_WIDTH


def log_sigmoid(x):
    return jnp.minimum(x, 0.0) - jnp.log1p(jnp.exp(-jnp.abs(x)))


def segment_kernel(
    tok, ctx, main, inv, offset, added, q_out, k_out, v_out, cf_out, cb_out, packet,
    ck, cv, ccf, ccb, kf, kb, ckf, ckb,
):
    kc = q_out.shape[1]
    vc = v_out.shape[1]
    heads = kc // ADDRESS_WIDTH
    ends = (0, kc, 2 * kc, 2 * kc + vc, 3 * kc + vc, 4 * kc + vc)
    expand = (iota((heads, kc), 0) == iota((heads, kc), 1) // ADDRESS_WIDTH).astype(F32)

    def prepare(size, row, shift_row, k_ref, v_ref, cf_ref, cb_ref, at, latent):
        rows = pl.ds(row, size)
        here = pl.ds(at, size)
        scale = inv[rows, :]

        def pre(n):
            cols = pl.ds(ends[n], ends[n + 1] - ends[n])
            return scale * main[rows, cols] + main[pl.ds(shift_row, 1), cols]

        if latent:
            q_out[here, :] = pre(0).astype(BF16)
        k_ref[here, :] = pre(1).astype(BF16)
        v_ref[here, :] = pre(2).astype(BF16)
        log_f = log_sigmoid(pre(3) + offset[...]) / smoothing
        log_b = log_sigmoid(pre(4) + offset[...]) / smoothing
        if latent:
            extra = jnp.dot(added[here, :], expand, precision=exact, preferred_element_type=F32)
            log_f = log_f + extra
            log_b = log_b + extra
        r, c = iota((size, size), 0), iota((size, size), 1)
        lower = (r >= c).astype(F32)
        upper = (r <= c).astype(F32)
        cf_ref[here, :] = jnp.dot(lower, log_f, precision=exact, preferred_element_type=F32)
        cb_ref[here, :] = jnp.dot(upper, log_b, precision=exact, preferred_element_type=F32)

    def segment(length, size, k_ref, v_ref, cf_ref, cb_ref, kf_ref, kb_ref, place):
        count = length // size

        def step(i, totals):
            run_f, run_b = totals
            late = pl.multiple_of((count - 1 - i) * size, size)
            soon = pl.multiple_of(i * size, size)
            cum = cf_ref[pl.ds(late, size), :]
            end = cum[size - 1 :, :]
            kf_ref[pl.ds(late, size), :] = (
                k_ref[pl.ds(late, size), :].astype(F32) * jnp.exp(run_f + end - cum)
            ).astype(BF16)
            cum_b = cb_ref[pl.ds(soon, size), :]
            end_b = cum_b[:1, :]
            kb_ref[pl.ds(soon, size), :] = (
                k_ref[pl.ds(soon, size), :].astype(F32) * jnp.exp(run_b + end_b - cum_b)
            ).astype(BF16)
            return run_f + end, run_b + end_b

        zero = jnp.zeros((1, kc), F32)
        totals = lax.fori_loop(0, count, step, (zero, zero))
        mask = diagonal_mask()
        for way, weighted in enumerate((kf_ref, kb_ref)):
            for g in range(heads // GROUP):
                full = outer(v_ref[:, g * GV : (g + 1) * GV], weighted[:, g * GK : (g + 1) * GK])
                full = jnp.where(mask, full, 0.0)
                state = full[:VALUE_DIM]
                for h in range(1, GROUP):
                    state = state + full[h * VALUE_DIM : (h + 1) * VALUE_DIM]
                packet[place + way, :VALUE_DIM, g * GK : (g + 1) * GK] = state.astype(BF16)
            high = totals[way].astype(BF16).astype(F32)
            low = totals[way] - high
            both = jnp.concatenate(
                [jnp.broadcast_to(high, (LOG_ROWS, kc)), jnp.broadcast_to(low, (LOG_ROWS, kc))], axis=0
            )
            packet[place + way, VALUE_DIM:, :] = both.astype(BF16)

    size = block_of(tok)
    csize = block_of(ctx)

    def latent_step(i, carry):
        at = pl.multiple_of(i * size, size)
        prepare(size, at, tok + ctx, k_out, v_out, cf_out, cb_out, at, True)
        return carry

    lax.fori_loop(0, tok // size, latent_step, 0)
    for i in range(ctx // csize):
        prepare(
            csize, tok + i * csize, tok + ctx + 1, ck, cv, ccf, ccb, i * csize, False
        )
    segment(tok, size, k_out, v_out, cf_out, cb_out, kf, kb, 0)
    segment(ctx, csize, ck, cv, ccf, ccb, ckf, ckb, 2)


def mixer_kernel(segments, q, k, v, cf, cb, packets, gain, out, state_f, state_b, saved):
    tok, kc = q.shape
    groups = kc // GK
    size = block_of(tok)
    count = tok // size
    half = size // 2
    place = lax.axis_index("sp")
    mask = diagonal_mask()

    def entering(way):
        def read(seg, kind):
            part = packets[seg, kind].astype(F32)
            logs = part[VALUE_DIM : VALUE_DIM + 1] + part[VALUE_DIM + LOG_ROWS : VALUE_DIM + LOG_ROWS + 1]
            return jnp.exp(logs), part[:VALUE_DIM]

        order = range(segments) if way == 0 else range(segments - 1, -1, -1)
        state = jnp.zeros((VALUE_DIM, kc), F32)
        for seg in order:
            decay, own = read(seg, 2 + way)
            state = decay * state + own
        for seg in order:
            decay, own = read(seg, way)
            active = seg < place if way == 0 else seg > place
            state = jnp.where(active, decay * state + own, state)
        return state

    for way, ref in ((0, state_f), (1, state_b)):
        state = entering(way)
        for g in range(groups):
            tiled = jnp.concatenate([state[:, g * GK : (g + 1) * GK]] * GROUP, axis=0)
            ref[g] = jnp.where(mask, tiled, 0.0)

    def advance(ref, g, end, cum, k_block, v_block):
        weighted = (k_block * jnp.exp(end - cum)).astype(BF16)
        ref[g] = ref[g] * jnp.exp(end) + jnp.where(mask, outer(v_block, weighted), 0.0)

    def back(i, carry):
        b = count - 1 - i
        rows = pl.ds(pl.multiple_of(b * size, size), size)
        for g in range(groups):
            saved[b, g] = state_b[g].astype(BF16)
            keys = slice(g * GK, (g + 1) * GK)
            cum = cb[rows, keys]
            advance(
                state_b, g, cum[:1], cum, k[rows, keys].astype(F32), v[rows, g * GV : (g + 1) * GV]
            )
        return carry

    lax.fori_loop(0, count, back, 0)

    key_head = iota((size, GK), 1) // ADDRESS_WIDTH
    value_head = iota((size, GV), 1) // VALUE_DIM
    row = iota((size, size), 0)
    col = iota((size, size), 1)
    lower = row >= col
    upper = row <= col
    ones = (iota((GV, GV), 0) // VALUE_DIM == iota((GV, GV), 1) // VALUE_DIM).astype(BF16)

    def ahead(b, carry):
        rows = pl.ds(pl.multiple_of(b * size, size), size)
        for g in range(groups):
            keys = slice(g * GK, (g + 1) * GK)
            q_block = q[rows, keys].astype(F32) * ADDRESS_WIDTH ** (-0.5)
            k_block = k[rows, keys].astype(F32)
            v_block = v[rows, g * GV : (g + 1) * GV]
            cum_f = cf[rows, keys]
            cum_b = cb[rows, keys]
            mid_f = cum_f[half - 1 : half]
            mid_b = cum_b[half : half + 1]
            q_f = (q_block * jnp.exp(cum_f - mid_f)).astype(BF16)
            k_f = (k_block * jnp.exp(mid_f - cum_f)).astype(BF16)
            q_b = (q_block * jnp.exp(cum_b - mid_b)).astype(BF16)
            k_b = (k_block * jnp.exp(mid_b - cum_b)).astype(BF16)
            mixed = contract((q_block * jnp.exp(cum_f)).astype(BF16), state_f[g].astype(BF16))
            mixed = mixed + contract((q_block * jnp.exp(cum_b)).astype(BF16), saved[b, g])
            for h in range(GROUP):
                zero = jnp.zeros_like(q_f)
                s_f = contract(jnp.where(key_head == h, q_f, zero), k_f)
                s_b = contract(jnp.where(key_head == h, q_b, zero), k_b)
                scores = jnp.where(lower, s_f, 0.0) + jnp.where(upper, s_b, 0.0)
                part = jnp.dot(scores.astype(BF16), v_block, preferred_element_type=F32)
                mixed = mixed + jnp.where(value_head == h, part, 0.0)
            advance(state_f, g, cum_f[size - 1 :], cum_f, k_block, v_block)
            square = mixed * mixed
            high = square.astype(BF16)
            low = (square - high.astype(F32)).astype(BF16)
            total = jnp.dot(high, ones, preferred_element_type=F32) + jnp.dot(
                low, ones, preferred_element_type=F32
            )
            normed = mixed * lax.rsqrt(total / VALUE_DIM + epsilon)
            values = slice(g * GV, (g + 1) * GV)
            out[rows, values] = (normed * gain[:, values]).astype(BF16)
        return carry

    lax.fori_loop(0, count, ahead, 0)


LIMIT = 56 * 1024 * 1024


def segments_of(tok, ctx, kc, vc, main, inv, offset, added):
    shape = jax.ShapeDtypeStruct
    return pl.pallas_call(
        functools.partial(segment_kernel, tok, ctx),
        out_shape=(
            shape((tok, kc), BF16),
            shape((tok, kc), BF16),
            shape((tok, vc), BF16),
            shape((tok, kc), F32),
            shape((tok, kc), F32),
            shape((4, VALUE_DIM + 2 * LOG_ROWS, kc), BF16),
        ),
        scratch_shapes=[
            pltpu.VMEM((ctx, kc), BF16),
            pltpu.VMEM((ctx, vc), BF16),
            pltpu.VMEM((ctx, kc), F32),
            pltpu.VMEM((ctx, kc), F32),
            pltpu.VMEM((tok, kc), BF16),
            pltpu.VMEM((tok, kc), BF16),
            pltpu.VMEM((ctx, kc), BF16),
            pltpu.VMEM((ctx, kc), BF16),
        ],
        compiler_params=pltpu.CompilerParams(vmem_limit_bytes=LIMIT),
        name="segments",
    )(main, inv, offset, added)


def mix(q, k, v, cf, cb, packets, gain):
    tok, kc = q.shape
    groups = kc // GK
    return pl.pallas_call(
        functools.partial(mixer_kernel, packets.shape[0]),
        out_shape=jax.ShapeDtypeStruct(v.shape, BF16),
        scratch_shapes=[
            pltpu.VMEM((groups, GV, GK), F32),
            pltpu.VMEM((groups, GV, GK), F32),
            pltpu.VMEM((tok // block_of(tok), groups, GV, GK), BF16),
        ],
        compiler_params=pltpu.CompilerParams(vmem_limit_bytes=LIMIT),
        name="mixer",
    )(q, k, v, cf, cb, packets, gain)


def per_device(
    latent, context, cond, ctx_cond, w_shift, w_scale, w_gate, norm_gain, w_query, w_key, w_value,
    w_decay_fwd, w_decay_bwd, forgetting_shift_vector, decay_log, head_gain, w_out,
):
    tok, ctx = latent.shape[0], context.shape[0]
    kc, vc = w_query.shape[0], w_value.shape[0]
    width = w_query.shape[1]
    rows = lax.all_gather(jnp.concatenate([latent, context], axis=0), "tp", axis=1, tiled=True)
    w_local = jnp.concatenate([w_query, w_key, w_value, w_decay_fwd, w_decay_bwd], axis=0)
    activations = jnp.stack([jax.nn.silu(cond), jax.nn.silu(ctx_cond)]).astype(BF16)
    partials = jnp.concatenate(
        [jnp.dot(activations, w, preferred_element_type=F32) for w in (w_shift, w_scale, w_gate)], axis=0
    )
    modulation = lax.psum(partials, "sp")
    factors = jnp.concatenate([norm_gain[None, :] * (1.0 + modulation[2:4]), modulation[:2]], axis=0)
    factors = lax.all_gather(factors, "tp", axis=1, tiled=True)
    wide = rows.astype(F32)
    inv = lax.rsqrt(jnp.sum(wide * wide, axis=1, keepdims=True) / width + epsilon)
    is_latent = lax.broadcasted_iota(jnp.int32, (tok + ctx, 1), 0) < tok
    scaled = (wide * jnp.where(is_latent, factors[0:1], factors[1:2])).astype(BF16)
    shifts = jnp.pad(factors[2:4].astype(BF16), ((0, PAD - 2), (0, 0)))
    main = contract(jnp.concatenate([scaled, shifts], axis=0), w_local)
    q, k, v, cf, cb, packet = segments_of(
        tok, ctx, kc, vc, main, inv, forgetting_shift_vector[None, :], decay_log
    )
    packets = lax.all_gather(packet, "sp", axis=0, tiled=False)
    head_rows = mix(q, k, v, cf, cb, packets, head_gain[None, :])
    projected = contract(lax.all_gather(head_rows, "tp", axis=1, tiled=True), w_out)
    return (modulation[4:5] * projected).astype(BF16)


def solution(mesh):
    return jax.shard_map(
        per_device,
        mesh=mesh,
        in_specs=(
            P("sp", "tp"), P("sp", "tp"), P("sp"), P("sp"), P("sp", "tp"), P("sp", "tp"), P("sp", "tp"),
            P("tp"), P("tp", None), P("tp", None), P("tp", None), P("tp", None), P("tp", None), P("tp"),
            P("sp", "tp"), P("tp"), P("tp", None),
        ),
        out_specs=P("sp", "tp"),
        check_vma=False,
    )
```

```python
import functools

import jax
import jax.numpy as jnp
from jax import lax
from jax.experimental import pallas as pl
from jax.experimental.pallas import tpu as pltpu
from jax.sharding import PartitionSpec as P

ADDRESS_WIDTH = 32
VALUE_DIM = 64
GROUP = 4
GK = GROUP * ADDRESS_WIDTH
GV = GROUP * VALUE_DIM
PAD = 16
LOG_ROWS = 8

epsilon = 1e-06
smoothing = 16.0
exact = lax.Precision.HIGHEST
F32 = jnp.float32
BF16 = jnp.bfloat16


def block_of(length):
    block = 128
    while length % block:
        block //= 2
    return block


def contract(left, right):
    return lax.dot_general(left, right, (((1,), (1,)), ((), ())), preferred_element_type=F32)


def outer(left, right):
    return lax.dot_general(left, right, (((0,), (0,)), ((), ())), preferred_element_type=F32)


def iota(shape, axis):
    return lax.broadcasted_iota(jnp.int32, shape, axis)


def diagonal_mask():
    return iota((GV, GK), 0) // VALUE_DIM == iota((GV, GK), 1) // ADDRESS_WIDTH


def log_sigmoid(x):
    return jnp.minimum(x, 0.0) - jnp.log1p(jnp.exp(-jnp.abs(x)))


def segment_kernel(
    tok, ctx, main_a, main_b, inv_a, inv_b, offset, added, q_out, k_out, v_out, cf_out, cb_out, packet,
    ck, cv, ccf, ccb, kf, kb, ckf, ckb,
):
    kc = q_out.shape[1]
    vc = v_out.shape[1]
    heads = kc // ADDRESS_WIDTH
    ends = (0, kc, 2 * kc, 2 * kc + vc, 3 * kc + vc, 4 * kc + vc)
    expand = (iota((heads, kc), 0) == iota((heads, kc), 1) // ADDRESS_WIDTH).astype(F32)

    def prepare(size, main, inv, row, shift_row, k_ref, v_ref, cf_ref, cb_ref, at, latent):
        rows = pl.ds(row, size)
        here = pl.ds(at, size)
        scale = inv[rows, :]

        def pre(n):
            cols = pl.ds(ends[n], ends[n + 1] - ends[n])
            return scale * main[rows, cols] + main_b[pl.ds(shift_row, 1), cols]

        if latent:
            q_out[here, :] = pre(0).astype(BF16)
        k_ref[here, :] = pre(1).astype(BF16)
        v_ref[here, :] = pre(2).astype(BF16)
        log_f = log_sigmoid(pre(3) + offset[...]) / smoothing
        log_b = log_sigmoid(pre(4) + offset[...]) / smoothing
        if latent:
            extra = jnp.dot(added[here, :], expand, precision=exact, preferred_element_type=F32)
            log_f = log_f + extra
            log_b = log_b + extra
        r, c = iota((size, size), 0), iota((size, size), 1)
        lower = (r >= c).astype(F32)
        upper = (r <= c).astype(F32)
        cf_ref[here, :] = jnp.dot(lower, log_f, precision=exact, preferred_element_type=F32)
        cb_ref[here, :] = jnp.dot(upper, log_b, precision=exact, preferred_element_type=F32)

    def segment(length, size, k_ref, v_ref, cf_ref, cb_ref, kf_ref, kb_ref, place):
        count = length // size

        def step(i, totals):
            run_f, run_b = totals
            late = pl.multiple_of((count - 1 - i) * size, size)
            soon = pl.multiple_of(i * size, size)
            cum = cf_ref[pl.ds(late, size), :]
            end = cum[size - 1 :, :]
            kf_ref[pl.ds(late, size), :] = (
                k_ref[pl.ds(late, size), :].astype(F32) * jnp.exp(run_f + end - cum)
            ).astype(BF16)
            cum_b = cb_ref[pl.ds(soon, size), :]
            end_b = cum_b[:1, :]
            kb_ref[pl.ds(soon, size), :] = (
                k_ref[pl.ds(soon, size), :].astype(F32) * jnp.exp(run_b + end_b - cum_b)
            ).astype(BF16)
            return run_f + end, run_b + end_b

        zero = jnp.zeros((1, kc), F32)
        totals = lax.fori_loop(0, count, step, (zero, zero))
        mask = diagonal_mask()
        for way, weighted in enumerate((kf_ref, kb_ref)):
            for g in range(heads // GROUP):
                full = outer(v_ref[:, g * GV : (g + 1) * GV], weighted[:, g * GK : (g + 1) * GK])
                full = jnp.where(mask, full, 0.0)
                state = full[:VALUE_DIM]
                for h in range(1, GROUP):
                    state = state + full[h * VALUE_DIM : (h + 1) * VALUE_DIM]
                packet[place + way, :VALUE_DIM, g * GK : (g + 1) * GK] = state.astype(BF16)
            high = totals[way].astype(BF16).astype(F32)
            low = totals[way] - high
            both = jnp.concatenate(
                [jnp.broadcast_to(high, (LOG_ROWS, kc)), jnp.broadcast_to(low, (LOG_ROWS, kc))], axis=0
            )
            packet[place + way, VALUE_DIM:, :] = both.astype(BF16)

    size = block_of(tok)
    csize = block_of(ctx)

    first = inv_a.shape[0]
    shift_row = tok - first + ctx

    def latent_steps(main, inv, start, stop):
        def step(i, carry):
            at = pl.multiple_of(i * size, size)
            row = pl.multiple_of(at - start, size)
            prepare(size, main, inv, row, shift_row, k_out, v_out, cf_out, cb_out, at, True)
            return carry

        lax.fori_loop(start // size, stop // size, step, 0)

    latent_steps(main_a, inv_a, 0, first)
    latent_steps(main_b, inv_b, first, tok)
    for i in range(ctx // csize):
        prepare(
            csize, main_b, inv_b, tok - first + i * csize, shift_row + 1, ck, cv, ccf, ccb, i * csize, False
        )
    segment(tok, size, k_out, v_out, cf_out, cb_out, kf, kb, 0)
    segment(ctx, csize, ck, cv, ccf, ccb, ckf, ckb, 2)


def mixer_kernel(segments, first, last, q, k, v, cf, cb, packets, gain, out, state_f, state_b, saved):
    tok, kc = q.shape
    groups = kc // GK
    size = block_of(tok)
    count = tok // size
    half = size // 2
    place = lax.axis_index("sp")
    mask = diagonal_mask()

    def entering(way):
        def read(seg, kind):
            part = packets[seg, kind].astype(F32)
            logs = part[VALUE_DIM : VALUE_DIM + 1] + part[VALUE_DIM + LOG_ROWS : VALUE_DIM + LOG_ROWS + 1]
            return jnp.exp(logs), part[:VALUE_DIM]

        order = range(segments) if way == 0 else range(segments - 1, -1, -1)
        state = jnp.zeros((VALUE_DIM, kc), F32)
        for seg in order:
            decay, own = read(seg, 2 + way)
            state = decay * state + own
        for seg in order:
            decay, own = read(seg, way)
            active = seg < place if way == 0 else seg > place
            state = jnp.where(active, decay * state + own, state)
        return state

    for way, ref in ((0, state_f), (1, state_b)):
        state = entering(way)
        for g in range(groups):
            tiled = jnp.concatenate([state[:, g * GK : (g + 1) * GK]] * GROUP, axis=0)
            ref[g] = jnp.where(mask, tiled, 0.0)

    def advance(ref, g, end, cum, k_block, v_block):
        weighted = (k_block * jnp.exp(end - cum)).astype(BF16)
        ref[g] = ref[g] * jnp.exp(end) + jnp.where(mask, outer(v_block, weighted), 0.0)

    def back(i, carry):
        b = count - 1 - i
        rows = pl.ds(pl.multiple_of(b * size, size), size)
        for g in range(groups):
            saved[b, g] = state_b[g].astype(BF16)
            keys = slice(g * GK, (g + 1) * GK)
            cum = cb[rows, keys]
            advance(
                state_b, g, cum[:1], cum, k[rows, keys].astype(F32), v[rows, g * GV : (g + 1) * GV]
            )
        return carry

    lax.fori_loop(0, count - first, back, 0)

    key_head = iota((size, GK), 1) // ADDRESS_WIDTH
    value_head = iota((size, GV), 1) // VALUE_DIM
    row = iota((size, size), 0)
    col = iota((size, size), 1)
    lower = row >= col
    upper = row <= col
    ones = (iota((GV, GV), 0) // VALUE_DIM == iota((GV, GV), 1) // VALUE_DIM).astype(BF16)

    def skip(b, carry):
        rows = pl.ds(pl.multiple_of(b * size, size), size)
        for g in range(groups):
            keys = slice(g * GK, (g + 1) * GK)
            cum = cf[rows, keys]
            advance(
                state_f, g, cum[size - 1 :], cum, k[rows, keys].astype(F32), v[rows, g * GV : (g + 1) * GV]
            )
        return carry

    lax.fori_loop(0, first, skip, 0)

    def ahead(b, carry):
        here = pl.ds(pl.multiple_of((b - first) * size, size), size)
        rows = pl.ds(pl.multiple_of(b * size, size), size)
        for g in range(groups):
            keys = slice(g * GK, (g + 1) * GK)
            q_block = q[rows, keys].astype(F32) * ADDRESS_WIDTH ** (-0.5)
            k_block = k[rows, keys].astype(F32)
            v_block = v[rows, g * GV : (g + 1) * GV]
            cum_f = cf[rows, keys]
            cum_b = cb[rows, keys]
            mid_f = cum_f[half - 1 : half]
            mid_b = cum_b[half : half + 1]
            q_f = (q_block * jnp.exp(cum_f - mid_f)).astype(BF16)
            k_f = (k_block * jnp.exp(mid_f - cum_f)).astype(BF16)
            q_b = (q_block * jnp.exp(cum_b - mid_b)).astype(BF16)
            k_b = (k_block * jnp.exp(mid_b - cum_b)).astype(BF16)
            mixed = contract((q_block * jnp.exp(cum_f)).astype(BF16), state_f[g].astype(BF16))
            mixed = mixed + contract((q_block * jnp.exp(cum_b)).astype(BF16), saved[b, g])
            for h in range(GROUP):
                zero = jnp.zeros_like(q_f)
                s_f = contract(jnp.where(key_head == h, q_f, zero), k_f)
                s_b = contract(jnp.where(key_head == h, q_b, zero), k_b)
                scores = jnp.where(lower, s_f, 0.0) + jnp.where(upper, s_b, 0.0)
                part = jnp.dot(scores.astype(BF16), v_block, preferred_element_type=F32)
                mixed = mixed + jnp.where(value_head == h, part, 0.0)
            advance(state_f, g, cum_f[size - 1 :], cum_f, k_block, v_block)
            square = mixed * mixed
            high = square.astype(BF16)
            low = (square - high.astype(F32)).astype(BF16)
            total = jnp.dot(high, ones, preferred_element_type=F32) + jnp.dot(
                low, ones, preferred_element_type=F32
            )
            normed = mixed * lax.rsqrt(total / VALUE_DIM + epsilon)
            values = slice(g * GV, (g + 1) * GV)
            out[here, values] = (normed * gain[:, values]).astype(BF16)
        return carry

    lax.fori_loop(first, last, ahead, 0)


LIMIT = 56 * 1024 * 1024


def segments_of(tok, ctx, kc, vc, *operands):
    shape = jax.ShapeDtypeStruct
    return pl.pallas_call(
        functools.partial(segment_kernel, tok, ctx),
        out_shape=(
            shape((tok, kc), BF16),
            shape((tok, kc), BF16),
            shape((tok, vc), BF16),
            shape((tok, kc), F32),
            shape((tok, kc), F32),
            shape((4, VALUE_DIM + 2 * LOG_ROWS, kc), BF16),
        ),
        scratch_shapes=[
            pltpu.VMEM((ctx, kc), BF16),
            pltpu.VMEM((ctx, vc), BF16),
            pltpu.VMEM((ctx, kc), F32),
            pltpu.VMEM((ctx, kc), F32),
            pltpu.VMEM((tok, kc), BF16),
            pltpu.VMEM((tok, kc), BF16),
            pltpu.VMEM((ctx, kc), BF16),
            pltpu.VMEM((ctx, kc), BF16),
        ],
        compiler_params=pltpu.CompilerParams(vmem_limit_bytes=LIMIT),
        name="segments",
    )(*operands)


def mix(first, last, q, k, v, cf, cb, packets, gain):
    tok, kc = q.shape
    groups = kc // GK
    return pl.pallas_call(
        functools.partial(mixer_kernel, packets.shape[0], first, last),
        out_shape=jax.ShapeDtypeStruct(((last - first) * block_of(tok), v.shape[1]), BF16),
        scratch_shapes=[
            pltpu.VMEM((groups, GV, GK), F32),
            pltpu.VMEM((groups, GV, GK), F32),
            pltpu.VMEM((tok // block_of(tok), groups, GV, GK), BF16),
        ],
        compiler_params=pltpu.CompilerParams(vmem_limit_bytes=LIMIT),
        name="mixer",
    )(q, k, v, cf, cb, packets, gain)


def spread_kernel(n, src, dst, send, recv, local):
    me = lax.axis_index("sp")
    barrier = pltpu.get_barrier_semaphore()
    for d in range(1, n):
        pl.semaphore_signal(
            barrier, inc=1, device_id={"sp": lax.rem(me + d, n)}, device_id_type=pl.DeviceIdType.MESH
        )
    pl.semaphore_wait(barrier, n - 1)
    copies = [pltpu.make_async_copy(src, dst.at[me], local)]
    for d in range(1, n):
        copies.append(
            pltpu.make_async_remote_copy(
                src_ref=src,
                dst_ref=dst.at[me],
                send_sem=send.at[d - 1],
                recv_sem=recv.at[d - 1],
                device_id={"sp": lax.rem(me + d, n)},
                device_id_type=pl.DeviceIdType.MESH,
            )
        )
    for copy in copies:
        copy.start()
    for copy in copies:
        copy.wait()


def spread(packet):
    n = lax.axis_size("sp")
    return pl.pallas_call(
        functools.partial(spread_kernel, n),
        out_shape=jax.ShapeDtypeStruct((n,) + packet.shape, packet.dtype),
        in_specs=[pl.BlockSpec(memory_space=pltpu.VMEM)],
        out_specs=pl.BlockSpec(memory_space=pltpu.VMEM),
        scratch_shapes=[
            pltpu.SemaphoreType.DMA((n - 1,)),
            pltpu.SemaphoreType.DMA((n - 1,)),
            pltpu.SemaphoreType.DMA,
        ],
        compiler_params=pltpu.CompilerParams(collective_id=0, has_side_effects=True),
        name="spread",
    )(packet)


def per_device(
    latent, context, cond, ctx_cond, w_shift, w_scale, w_gate, norm_gain, w_query, w_key, w_value,
    w_decay_fwd, w_decay_bwd, forgetting_shift_vector, decay_log, head_gain, w_out,
):
    tok, ctx = latent.shape[0], context.shape[0]
    kc, vc = w_query.shape[0], w_value.shape[0]
    width = w_query.shape[1]
    size = block_of(tok)
    count = tok // size
    first = count // 2 * size
    rows_a = lax.all_gather(latent[:first], "tp", axis=1, tiled=True)
    rows_b = lax.all_gather(
        jnp.concatenate([latent[first:], context], axis=0), "tp", axis=1, tiled=True
    )
    w_local = jnp.concatenate([w_query, w_key, w_value, w_decay_fwd, w_decay_bwd], axis=0)
    activations = jnp.stack([jax.nn.silu(cond), jax.nn.silu(ctx_cond)]).astype(BF16)
    partials = jnp.concatenate(
        [jnp.dot(activations, w, preferred_element_type=F32) for w in (w_shift, w_scale, w_gate)], axis=0
    )
    modulation = lax.psum(partials, "sp")
    factors = jnp.concatenate([norm_gain[None, :] * (1.0 + modulation[2:4]), modulation[:2]], axis=0)
    factors = lax.all_gather(factors, "tp", axis=1, tiled=True)

    def inverse(wide):
        return lax.rsqrt(jnp.sum(wide * wide, axis=1, keepdims=True) / width + epsilon)

    wide_a = rows_a.astype(F32)
    wide_b = rows_b.astype(F32)
    is_latent = lax.broadcasted_iota(jnp.int32, (tok - first + ctx, 1), 0) < tok - first
    scaled_a = (wide_a * factors[0:1]).astype(BF16)
    scaled_b = (wide_b * jnp.where(is_latent, factors[0:1], factors[1:2])).astype(BF16)
    shifts = jnp.pad(factors[2:4].astype(BF16), ((0, PAD - 2), (0, 0)))
    main_a = contract(scaled_a, w_local)
    main_b = contract(jnp.concatenate([scaled_b, shifts], axis=0), w_local)
    q, k, v, cf, cb, packet = segments_of(
        tok, ctx, kc, vc, main_a, main_b, inverse(wide_a), inverse(wide_b),
        forgetting_shift_vector[None, :], decay_log,
    )
    packets = spread(packet)
    parts = []
    for begin, end in ((0, count // 2), (count // 2, count)):
        head_rows = mix(begin, end, q, k, v, cf, cb, packets, head_gain[None, :])
        projected = contract(lax.all_gather(head_rows, "tp", axis=1, tiled=True), w_out)
        parts.append((modulation[4:5] * projected).astype(BF16))
    return jnp.concatenate(parts, axis=0)


def solution(mesh):
    return jax.shard_map(
        per_device,
        mesh=mesh,
        in_specs=(
            P("sp", "tp"), P("sp", "tp"), P("sp"), P("sp"), P("sp", "tp"), P("sp", "tp"), P("sp", "tp"),
            P("tp"), P("tp", None), P("tp", None), P("tp", None), P("tp", None), P("tp", None), P("tp"),
            P("sp", "tp"), P("tp"), P("tp", None),
        ),
        out_specs=P("sp", "tp"),
        check_vma=False,
    )
```
